32 devices in a mesh: sp: 8 (over z, x), tp: 4 (over y, core).
Axes of the slice: x: 2, y: 2, z: 4, core: 2. Of those that a mesh axis runs over, the one named last changes fastest.
Arguments:
- resid: bfloat16 [1024, 2048], P('sp'), may hold values from -8 to 8
- a_val: bfloat16 [1024, 1024], P('sp', 'tp'), may hold values from -8 to 8
- a_gate: bfloat16 [1024, 1024], P('sp', 'tp'), may hold values from -6 to 6
- conv_kernel: bfloat16 [31, 1024], P(None, 'tp'), may hold values from -1 to 1
- conv_bias: float32 [1024], P('tp'), may hold values from -3 to 3
- ln_gain: float32 [1024], P('tp'), may hold values from 0.1 to 1.9
- ln_bias: float32 [1024], P('tp'), may hold values from -3 to 3
- w_out: bfloat16 [1024, 2048], P('tp'), may hold values from -0.1875 to 0.1875
- ffn_gain: float32 [2048], replicated, may hold values from 0.1 to 1.9
- routes: int32 [1024, 4], P('sp'), may hold values from 0 to 7, all different within a row; in each aligned block of 128 rows (0 to 127, 128 to 255, ...) at most 128 rows name the same one
- route_weights: float32 [1024, 4], P('sp'), may hold values from 0.15 to 1.2
- exp_gate: bfloat16 [8, 2048, 4096], P('sp', None, 'tp'), may hold values from -0.125 to 0.125
- exp_up: bfloat16 [8, 2048, 4096], P('sp', None, 'tp'), may hold values from -0.125 to 0.125
- exp_down: bfloat16 [8, 4096, 2048], P('sp', None, 'tp'), may hold values from -0.09375 to 0.09375
- sh_gate: bfloat16 [2048, 512], P(None, 'tp'), may hold values from -0.125 to 0.125
- sh_up: bfloat16 [2048, 512], P(None, 'tp'), may hold values from -0.125 to 0.125
- sh_down: bfloat16 [512, 2048], P(None, 'tp'), may hold values from -0.25 to 0.25
Outputs:
- result: bfloat16 [1024, 2048], P('sp', 'tp')
The draws below stay inside these ranges and needn't reach their ends.
Inputs may be any that keep to these rules, and one draw needn't show every extreme that they name: `routes`: among the 128 rows of one index of sp, each expert is named at most 128 times, a bound that some block reaches; a row names 4 different experts.
All inputs are finite; a program needn't handle non-finite values.
Results may differ from the reference program's by a relative error of at most 0.007.
Values may be sent and summed in bfloat16 or wider, within the bound.
A program may use at most 64 MiB of HBM per device.

```python
import math
import jax
import jax.numpy as jnp
import numpy as np
from jax import lax

D = 2048
D_A = 1024
D_E = 4096
D_S = 512
CONV_SPAN = 31
TOPK = 4
TOK_SP = 128
EXPERTS = 8
TOKENS = 1024
CAP = 128
N_SP = 8


def rising_field(key, row_count, col_count, lowest, growth):
    subkeys = jax.random.split(jax.random.fold_in(key, 11), 2)
    position = jnp.arange(col_count, dtype=jnp.float32) / col_count
    roughness = jnp.exp(jax.random.uniform(subkeys[1], (col_count,), jnp.float32, -0.35, 0.35))
    values = jax.random.normal(subkeys[0], (row_count, col_count), jnp.float32)
    drawn = values * (lowest * growth ** position * roughness)[None, :]
    return jnp.clip(drawn, -8.0, 8.0)


def draw_resid(key, part):
    return rising_field(jax.random.fold_in(key, 3), TOKENS, D, 0.5, 3.0).astype(jnp.bfloat16)


def draw_a_val(key, part):
    return rising_field(jax.random.fold_in(key, 5), TOKENS, D_A, 0.5, 3.0).astype(jnp.bfloat16)


def shard_levels(rng, dims, cuts, low, top_value):
    level = 1.0
    for axis_at, shards_of in cuts:
        steps = jax.random.uniform(jax.random.fold_in(jax.random.fold_in(rng, 6), axis_at), (shards_of,), jnp.float32, low / len(cuts), top_value / len(cuts))
        level = level * jnp.repeat(jnp.exp(steps), dims[axis_at] // shards_of).reshape((-1,) + (1,) * (len(dims) - 1 - axis_at))
    return level


def deal_out(rng, own, number, rows, amount, top, limit, skew):
    order = jax.random.permutation(rng, amount)
    crowded, usual = load_shares(amount, rows * top, limit, skew, True), load_shares(amount, rows * top, limit, skew, False)
    places = jnp.arange(amount)

    def named(tallies, offset_by):
        used = int((tallies > 0).sum())
        fixed = max(1, used // 4)
        passed = fixed + (places - fixed + offset_by * (used - fixed)) % max(1, amount - fixed)
        return jnp.zeros((amount,), jnp.int32).at[order[jnp.where(places < fixed, places, passed)]].set(jnp.asarray(tallies, jnp.int32))

    tallies = jnp.where(number % 4 == 0, named(crowded, number // 4), named(usual, number - number // 4 - 1))
    mixed = jax.random.permutation(jax.random.fold_in(own, 3), amount)
    source_of, sink = mixed[0:amount // 2 * 2:2], mixed[1:amount // 2 * 2:2]
    margin = jnp.minimum(tallies[source_of] - 1, limit - tallies[sink]) // 2
    margin = jnp.where((source_of == order[0]) | (sink == order[0]) | (tallies[sink] == 0), 0, jnp.maximum(margin, 0))
    passed = jax.random.randint(jax.random.fold_in(own, 4), (amount // 2,), 0, 1 << 20) % (margin + 1)
    tallies = tallies.at[source_of].add(-passed).at[sink].add(passed)
    labels = jnp.searchsorted(jnp.cumsum(tallies), jnp.arange(rows * top), side="right").astype(jnp.int32)
    table = labels.reshape(top, rows).T
    table = table[jax.random.permutation(jax.random.fold_in(own, 1), rows)]
    offset_by = jax.random.randint(jax.random.fold_in(own, 2), (rows, 1), 0, top)
    return jnp.take_along_axis(table, (jnp.arange(top)[None, :] + offset_by) % top, axis=1)


def load_shares(count, total, limit, lean, full):
    weights = [(1 << 20) // math.isqrt(grade ** lean) + 1 for grade in range(1, count + 1)]
    largest = limit if full else min(limit, max(-(-total // count), total * weights[0] // sum(weights)))
    least = 1 if total - largest >= count - 1 else 0
    holding, spare = [largest] + [least] * (count - 1), total - largest - least * (count - 1)
    while spare > 0:
        movable = [i for i in range(1, count) if holding[i] < largest] or [i for i in range(1, count) if holding[i] < limit]
        pool, remaining = sum([weights[i] for i in movable]), spare
        for i in movable:
            addition = min(limit - holding[i], max(1, remaining * weights[i] // pool), spare)
            holding[i] = holding[i] + addition
            spare = spare - addition
    return np.array(holding)


def normal_values(key, shape, spread, limit, cuts=(), kind=jnp.bfloat16):
    values = jax.random.normal(key, shape, jnp.float32) * spread
    if len(cuts) > 0:
        values = shard_levels(key, shape, cuts, -0.22, 0.18) * values
    return jnp.clip(values, min=-limit, max=limit).astype(kind)


def setup_inputs(seed: int = 0) -> dict:
    streams_of = jax.random.split(jax.random.key(seed), 18)
    resid = draw_resid(jax.random.fold_in(streams_of[17], 71), 0)
    a_val = draw_a_val(jax.random.fold_in(streams_of[17], 71), 0)
    a_gate = normal_values(streams_of[2], (TOKENS, D_A), 1.0, 6.0, ((0, 8), (1, 4)))
    conv_kernel = normal_values(streams_of[3], (CONV_SPAN, D_A), CONV_SPAN ** -0.5, 1.0, ((1, 4),))
    conv_bias = normal_values(streams_of[4], (D_A,), 0.5, 3.0, ((0, 4),), jnp.float32)
    ln_gain = jnp.clip(1.0 + 0.18 * jax.random.normal(streams_of[5], (D_A,), jnp.float32), 0.1, 1.9)
    ln_bias = normal_values(streams_of[6], (D_A,), 0.5, 3.0, ((0, 4),), jnp.float32)
    w_out = normal_values(streams_of[7], (D_A, D), D_A ** -0.5, 0.1875, ((0, 4),))
    ffn_gain = jnp.clip(1.0 + 0.18 * jax.random.normal(streams_of[8], (D,), jnp.float32), 0.1, 1.9)
    routes_keys = jax.random.split(jax.random.fold_in(streams_of[9], 1), TOKENS // TOK_SP)
    routes_turns = jax.random.permutation(jax.random.fold_in(streams_of[9], 3), TOKENS // TOK_SP)
    routes = jax.vmap(lambda own, number: deal_out(jax.random.fold_in(streams_of[9], 2), own, number, TOK_SP, EXPERTS, TOPK, CAP, 1))(routes_keys, routes_turns).reshape((TOKENS, TOPK))
    route_weights = jnp.clip(jnp.exp(math.log(1.2) - 2.0794415 * jax.random.uniform(streams_of[10], (TOKENS, TOPK), jnp.float32) ** shard_levels(streams_of[10], (TOKENS, TOPK), ((0, 8),), -0.2, 0.2)), 0.15, 1.2)
    exp_gate = normal_values(streams_of[11], (EXPERTS, D, D_E), D ** -0.5, 0.125, ((0, 8), (2, 4)))
    exp_up = normal_values(streams_of[12], (EXPERTS, D, D_E), D ** -0.5, 0.125, ((0, 8), (2, 4)))
    exp_down = normal_values(streams_of[13], (EXPERTS, D_E, D), D_E ** -0.5, 0.09375, ((0, 8), (2, 4)))
    sh_gate = normal_values(streams_of[14], (D, D_S), D ** -0.5, 0.125, ((1, 4),))
    sh_up = normal_values(streams_of[15], (D, D_S), D ** -0.5, 0.125, ((1, 4),))
    sh_down = normal_values(streams_of[16], (D_S, D), D_S ** -0.5, 0.25, ((1, 4),))
    return dict(resid=resid, a_val=a_val, a_gate=a_gate, conv_kernel=conv_kernel, conv_bias=conv_bias, ln_gain=ln_gain, ln_bias=ln_bias, w_out=w_out, ffn_gain=ffn_gain, routes=routes, route_weights=route_weights, exp_gate=exp_gate, exp_up=exp_up, exp_down=exp_down, sh_gate=sh_gate, sh_up=sh_up, sh_down=sh_down)


LN_EPS = 1e-05
RMS_EPS = 1e-06

def reference(resid, a_val, a_gate, conv_kernel, conv_bias, ln_gain, ln_bias, w_out, ffn_gain, routes, route_weights, exp_gate, exp_up, exp_down, sh_gate, sh_up, sh_down):
    gated_in = (a_val.astype(jnp.float32) * jax.nn.sigmoid(a_gate.astype(jnp.float32))).astype(jnp.bfloat16)
    padded = jnp.pad(gated_in, ((CONV_SPAN - 1, 0), (0, 0))).astype(jnp.float32)
    kernel = conv_kernel.astype(jnp.float32)

    def add_tap(offset, running):
        window_rows = lax.dynamic_slice_in_dim(padded, offset, TOKENS, 0)
        return running + lax.dynamic_slice_in_dim(kernel, offset, 1, 0) * window_rows
    start_sum = jnp.broadcast_to(conv_bias[None, :], (TOKENS, D_A)).astype(jnp.float32)
    conv_out = lax.fori_loop(0, CONV_SPAN, add_tap, start_sum)
    channel_mean = lax.optimization_barrier(jnp.mean(conv_out, axis=1, keepdims=True))
    channel_var = lax.optimization_barrier(jnp.mean(conv_out * conv_out, axis=1, keepdims=True)) - channel_mean * channel_mean
    scaled = (conv_out - channel_mean) * lax.rsqrt(channel_var + LN_EPS) * ln_gain[None, :] + ln_bias[None, :]
    mixed_out = jax.nn.silu(scaled).astype(jnp.bfloat16)
    projected = jnp.dot(mixed_out, w_out, preferred_element_type=jnp.float32)
    middle = (resid.astype(jnp.float32) + projected).astype(jnp.bfloat16)
    middle_f = middle.astype(jnp.float32)
    inverse = lax.rsqrt(lax.optimization_barrier(jnp.mean(middle_f * middle_f, axis=1, keepdims=True)) + RMS_EPS)
    normed = (middle_f * inverse * ffn_gain[None, :]).astype(jnp.bfloat16)
    shared_gate = jnp.dot(normed, sh_gate, preferred_element_type=jnp.float32)
    shared_up = jnp.dot(normed, sh_up, preferred_element_type=jnp.float32)
    shared_hidden = (jax.nn.silu(shared_gate) * shared_up).astype(jnp.bfloat16)
    shared = jnp.dot(shared_hidden, sh_down, preferred_element_type=jnp.float32)
    pair_count = TOK_SP * TOPK
    chosen_all = routes.reshape(N_SP, pair_count)
    expert_ids = jnp.arange(EXPERTS, dtype=jnp.int32)

    def block_places(chosen):
        one_hot = (chosen[:, None] == expert_ids[None, :]).astype(jnp.int32)
        earlier = jnp.cumsum(one_hot, axis=0) - one_hot
        return lax.optimization_barrier(jnp.sum(earlier * one_hot, axis=1)).astype(jnp.int32)
    place_in = lax.map(block_places, chosen_all)
    source_ids = jnp.arange(N_SP, dtype=jnp.int32)[:, None]
    target = source_ids * (EXPERTS * CAP) + chosen_all * CAP + place_in
    pair_ids = source_ids * pair_count + jnp.arange(pair_count, dtype=jnp.int32)[None, :]
    owner_ids = jnp.zeros((N_SP * EXPERTS * CAP,), jnp.int32).at[target.reshape(-1)].set(pair_ids.reshape(-1) + 1)
    owner_ids = owner_ids.reshape(N_SP, EXPERTS, CAP).transpose(1, 0, 2)

    def run_expert(packed):
        owners, gate_weight, up_weight, down_weight = packed
        flat_owner = owners.reshape(-1)
        source_row = jnp.maximum(flat_owner - 1, 0) // TOPK
        rows_in = jnp.where((flat_owner > 0)[:, None], normed[source_row], jnp.zeros((), jnp.bfloat16))
        gate_part = jnp.dot(rows_in, gate_weight, preferred_element_type=jnp.float32)
        up_part = jnp.dot(rows_in, up_weight, preferred_element_type=jnp.float32)
        hidden = (jax.nn.silu(gate_part) * up_part).astype(jnp.bfloat16)
        return jnp.dot(hidden, down_weight, preferred_element_type=jnp.float32).astype(jnp.bfloat16)
    expert_out = lax.map(run_expert, (owner_ids, exp_gate, exp_up, exp_down))
    flat_index = (chosen_all * (N_SP * CAP) + source_ids * CAP + place_in).reshape(-1)
    flat_out = expert_out.reshape(EXPERTS * N_SP * CAP, D)
    routed = jnp.zeros((TOKENS, D), jnp.float32)
    index_grid = flat_index.reshape(TOKENS, TOPK)
    for choice_k in range(TOPK):
        picked = flat_out[index_grid[:, choice_k]].astype(jnp.float32)
        routed = routed + route_weights[:, choice_k][:, None] * picked
    return (middle_f + shared + routed).astype(jnp.bfloat16)
```

```python
import jax
import jax.numpy as jnp
from jax import lax
from jax.sharding import PartitionSpec as P

LN_EPS = 1e-05
RMS_EPS = 1e-06


def shifted(value, axis, by):
    size = lax.axis_size(axis)
    pairs = [(i, i + by) for i in range(size) if 0 <= i + by < size]
    return lax.ppermute(value, axis, pairs)


def body_slots(
    resid,
    a_val,
    a_gate,
    conv_kernel,
    conv_bias,
    ln_gain,
    ln_bias,
    w_out,
    ffn_gain,
    routes,
    route_weights,
    exp_gate,
    exp_up,
    exp_down,
    sh_gate,
    sh_up,
    sh_down,
):
    tp_count = lax.axis_size("tp")
    tp_place = lax.axis_index("tp")
    sp_count = lax.axis_size("sp")
    tok_rows = resid.shape[0]
    model_width = resid.shape[1]
    col_width = model_width // tp_count
    col_start = tp_place * col_width
    conv_span = conv_kernel.shape[0]
    channels_all = a_val.shape[1] * tp_count
    gated_in = (a_val.astype(jnp.float32) * jax.nn.sigmoid(a_gate.astype(jnp.float32))).astype(
        jnp.bfloat16
    )
    before = shifted(gated_in[tok_rows - (conv_span - 1) :], "sp", 1)
    padded = jnp.concatenate([before, gated_in], axis=0).astype(jnp.float32)
    kernel = conv_kernel.astype(jnp.float32)

    def add_tap(offset, running):
        window_rows = lax.dynamic_slice_in_dim(padded, offset, tok_rows, 0)
        return running + lax.dynamic_slice_in_dim(kernel, offset, 1, 0) * window_rows

    start_sum = jnp.broadcast_to(conv_bias[None, :], gated_in.shape)
    conv_out = lax.fori_loop(0, conv_span, add_tap, start_sum)
    row_sums = lax.psum((jnp.sum(conv_out, axis=1), jnp.sum(conv_out * conv_out, axis=1)), "tp")
    channel_mean = row_sums[0] / channels_all
    channel_var = row_sums[1] / channels_all - channel_mean * channel_mean
    scaled = (conv_out - channel_mean[:, None]) * lax.rsqrt(
        channel_var[:, None] + LN_EPS
    ) * ln_gain[None, :] + ln_bias[None, :]
    mixed_out = jax.nn.silu(scaled).astype(jnp.bfloat16)
    partial_proj = jnp.dot(mixed_out, w_out, preferred_element_type=jnp.float32)
    projected = lax.psum(partial_proj, "tp")
    middle = (resid.astype(jnp.float32) + projected).astype(jnp.bfloat16)
    middle_f = middle.astype(jnp.float32)
    inverse = lax.rsqrt(jnp.mean(middle_f * middle_f, axis=1, keepdims=True) + RMS_EPS)
    normed = (middle_f * inverse * ffn_gain[None, :]).astype(jnp.bfloat16)
    middle_cols = lax.dynamic_slice_in_dim(middle, col_start, col_width, 1)
    shared_gate = jnp.dot(normed, sh_gate, preferred_element_type=jnp.float32)
    shared_up = jnp.dot(normed, sh_up, preferred_element_type=jnp.float32)
    shared_hidden = (jax.nn.silu(shared_gate) * shared_up).astype(jnp.bfloat16)
    weight_rows = sh_down
    shared = jnp.dot(
        lax.all_gather(shared_hidden, "tp", axis=1, tiled=True),
        weight_rows,
        preferred_element_type=jnp.float32,
    )
    top_count = routes.shape[1]
    local_experts = exp_gate.shape[0]
    experts_all = local_experts * sp_count
    capacity = max(2 * tok_rows * top_count // experts_all, tp_count)
    pair_count = tok_rows * top_count
    chosen = routes.reshape(pair_count)
    one_hot = (chosen[:, None] == jnp.arange(experts_all, dtype=jnp.int32)[None, :]).astype(
        jnp.int32
    )
    earlier = jnp.cumsum(one_hot, axis=0) - one_hot
    place_in = jnp.sum(earlier * one_hot, axis=1)
    slot_of = chosen * capacity + place_in
    owner_ids = (
        jnp.zeros((experts_all * capacity,), jnp.int32)
        .at[slot_of]
        .set(jnp.arange(pair_count, dtype=jnp.int32) + 1)
    )
    owner_grid = owner_ids.reshape(sp_count, local_experts, capacity)
    part_slots = capacity // tp_count
    own_owners = lax.dynamic_slice_in_dim(owner_grid, tp_place * part_slots, part_slots, 2)
    source_row = jnp.maximum(own_owners - 1, 0) // top_count
    taken = normed[source_row.reshape(-1)].reshape(own_owners.shape + (model_width,))
    landed = lax.all_to_all(
        jnp.where((own_owners > 0)[..., None], taken, jnp.zeros((), jnp.bfloat16)),
        "sp",
        split_axis=0,
        concat_axis=0,
        tiled=True,
    )
    arrived = lax.all_gather(landed, "tp", axis=2, tiled=True)
    gate_part = jnp.einsum("sxcd,xdf->sxcf", arrived, exp_gate, preferred_element_type=jnp.float32)
    up_part = jnp.einsum("sxcd,xdf->sxcf", arrived, exp_up, preferred_element_type=jnp.float32)
    expert_hidden = (jax.nn.silu(gate_part) * up_part).astype(jnp.bfloat16)
    weight_rows = exp_down
    expert_sum = jnp.einsum(
        "sxcf,xfd->sxcd",
        lax.all_gather(expert_hidden, "tp", axis=3, tiled=True),
        weight_rows,
        preferred_element_type=jnp.float32,
    )
    expert_out = expert_sum.astype(jnp.bfloat16)
    returned = lax.all_to_all(expert_out, "sp", split_axis=0, concat_axis=0, tiled=True)
    flat_out = returned.reshape(experts_all * capacity, col_width)
    picked = flat_out[slot_of].astype(jnp.float32).reshape(tok_rows, top_count, col_width)
    routed = jnp.sum(picked * route_weights[:, :, None], axis=1)
    return (middle_cols.astype(jnp.float32) + shared + routed).astype(jnp.bfloat16)


def swapped(value, axis, bit):
    size = lax.axis_size(axis)
    return lax.ppermute(value, axis, [(i, i ^ bit) for i in range(size)])


def body_dense(
    resid,
    a_val,
    a_gate,
    conv_kernel,
    conv_bias,
    ln_gain,
    ln_bias,
    w_out,
    ffn_gain,
    routes,
    route_weights,
    exp_gate,
    exp_up,
    exp_down,
    sh_gate,
    sh_up,
    sh_down,
):
    tp_count = lax.axis_size("tp")
    tp_place = lax.axis_index("tp")
    core = tp_place % 2
    row = tp_place // 2
    sp_count = lax.axis_size("sp")
    tok_rows, model_width = resid.shape
    col_width = model_width // tp_count
    half_width = model_width // 2
    part_hidden = exp_gate.shape[2]
    conv_span = conv_kernel.shape[0]
    channels_all = a_val.shape[1] * tp_count

    other_rows = lax.dynamic_slice_in_dim(exp_down[0], (1 - row) * 2 * part_hidden, 2 * part_hidden, 0)
    swapped_down = swapped(other_rows, "tp", 2)

    gated_in = (a_val.astype(jnp.float32) * jax.nn.sigmoid(a_gate.astype(jnp.float32))).astype(
        jnp.bfloat16
    )
    before = shifted(gated_in[tok_rows - (conv_span - 1) :], "sp", 1)
    expert_ids = jnp.arange(sp_count, dtype=jnp.int32)
    weight_mat = jnp.sum(
        jnp.where(routes[:, :, None] == expert_ids[None, None, :], route_weights[:, :, None], 0.0),
        axis=1,
    )
    weight_all = lax.all_gather(weight_mat, "sp", axis=0, tiled=True)
    weight_own = lax.dynamic_slice_in_dim(weight_all, lax.axis_index("sp"), 1, 1)
    padded = jnp.concatenate([before, gated_in], axis=0).astype(jnp.float32)
    kernel = conv_kernel.astype(jnp.float32)
    conv_out = jnp.broadcast_to(conv_bias[None, :], gated_in.shape)
    for tap in range(conv_span):
        conv_out = conv_out + kernel[tap : tap + 1] * padded[tap : tap + tok_rows]
    row_sums = lax.psum((jnp.sum(conv_out, axis=1), jnp.sum(conv_out * conv_out, axis=1)), "tp")
    channel_mean = row_sums[0] / channels_all
    channel_var = row_sums[1] / channels_all - channel_mean * channel_mean
    scaled = (conv_out - channel_mean[:, None]) * lax.rsqrt(
        channel_var[:, None] + LN_EPS
    ) * ln_gain[None, :] + ln_bias[None, :]
    mixed_out = jax.nn.silu(scaled).astype(jnp.bfloat16)
    partial_proj = jnp.dot(mixed_out, w_out, preferred_element_type=jnp.float32)
    give = lax.dynamic_slice_in_dim(partial_proj, (1 - core) * half_width, half_width, 1)
    keep = lax.dynamic_slice_in_dim(partial_proj, core * half_width, half_width, 1)
    chip_sum = keep + swapped(give.astype(jnp.bfloat16), "tp", 1).astype(jnp.float32)
    chip_sum = chip_sum.astype(jnp.bfloat16)
    half_sum = chip_sum.astype(jnp.float32) + swapped(chip_sum, "tp", 2).astype(jnp.float32)
    resid_half = lax.dynamic_slice_in_dim(resid, core * half_width, half_width, 1)
    mid_half = (resid_half.astype(jnp.float32) + half_sum).astype(jnp.bfloat16)
    mid_all = lax.all_gather(mid_half, "sp", axis=0, tiled=True)
    mid_peer = swapped(mid_half, "tp", 1)
    first = jnp.where(core == 0, mid_half, mid_peer)
    second = jnp.where(core == 0, mid_peer, mid_half)
    middle = jnp.concatenate([first, second], axis=1)

    middle_f = middle.astype(jnp.float32)
    inverse = lax.rsqrt(jnp.mean(middle_f * middle_f, axis=1, keepdims=True) + RMS_EPS)
    normed = (middle_f * inverse * ffn_gain[None, :]).astype(jnp.bfloat16)
    middle_cols = lax.dynamic_slice_in_dim(middle, tp_place * col_width, col_width, 1)
    shared_gate = jnp.dot(normed, sh_gate, preferred_element_type=jnp.float32)
    shared_up = jnp.dot(normed, sh_up, preferred_element_type=jnp.float32)
    shared_hidden = (jax.nn.silu(shared_gate) * shared_up).astype(jnp.bfloat16)
    shared = jnp.dot(
        lax.all_gather(shared_hidden, "tp", axis=1, tiled=True),
        sh_down,
        preferred_element_type=jnp.float32,
    )

    mid_all_peer = swapped(mid_all, "tp", 1)
    rows_first = jnp.where(core == 0, mid_all, mid_all_peer)
    rows_second = jnp.where(core == 0, mid_all_peer, mid_all)
    rows_f = jnp.concatenate([rows_first, rows_second], axis=1).astype(jnp.float32)
    rows_inverse = lax.rsqrt(jnp.mean(rows_f * rows_f, axis=1, keepdims=True) + RMS_EPS)
    rows = (rows_f * rows_inverse * ffn_gain[None, :]).astype(jnp.bfloat16)
    gate_part = jnp.dot(rows, exp_gate[0], preferred_element_type=jnp.float32)
    up_part = jnp.dot(rows, exp_up[0], preferred_element_type=jnp.float32)
    hidden = (jax.nn.silu(gate_part) * up_part).astype(jnp.bfloat16)
    hidden_peer = swapped(hidden, "tp", 1)

    own_at = tp_place * part_hidden
    peer_at = (tp_place ^ 1) * part_hidden
    stay = lax.dynamic_slice_in_dim
    out_own = jnp.dot(
        hidden, stay(exp_down[0], own_at, part_hidden, 0), preferred_element_type=jnp.float32
    ) + jnp.dot(
        hidden_peer, stay(exp_down[0], peer_at, part_hidden, 0), preferred_element_type=jnp.float32
    )
    out_far = jnp.dot(
        hidden, stay(swapped_down, core * part_hidden, part_hidden, 0), preferred_element_type=jnp.float32
    ) + jnp.dot(
        hidden_peer,
        stay(swapped_down, (1 - core) * part_hidden, part_hidden, 0),
        preferred_element_type=jnp.float32,
    )
    both = jnp.concatenate([out_own * weight_own, out_far * weight_own], axis=1).astype(jnp.bfloat16)
    summed = lax.psum_scatter(both, "sp", scatter_dimension=0, tiled=True)
    far = swapped(summed[:, col_width:], "tp", 2)
    routed = summed[:, :col_width].astype(jnp.float32) + far.astype(jnp.float32)
    return (middle_cols.astype(jnp.float32) + shared + routed).astype(jnp.bfloat16)


def body(*args):
    tok_rows = args[0].shape[0]
    top_count = args[9].shape[1]
    local_experts = args[11].shape[0]
    experts_all = local_experts * lax.axis_size("sp")
    capacity = 2 * tok_rows * top_count // experts_all
    if local_experts == 1 and lax.axis_size("tp") == 4 and capacity >= tok_rows:
        return body_dense(*args)
    return body_slots(*args)


def solution(mesh):
    in_specs = (
        P("sp", None),
        P("sp", "tp"),
        P("sp", "tp"),
        P(None, "tp"),
        P("tp"),
        P("tp"),
        P("tp"),
        P("tp", None),
        P(),
        P("sp", None),
        P("sp", None),
        P("sp", None, "tp"),
        P("sp", None, "tp"),
        P("sp", None, "tp"),
        P(None, "tp"),
        P(None, "tp"),
        P(None, "tp"),
    )
    out_specs = P("sp", "tp")
    return jax.shard_map(body, mesh=mesh, in_specs=in_specs, out_specs=out_specs, check_vma=False)
```

```python
import functools

import jax
import jax.numpy as jnp
from jax import lax
from jax.experimental import pallas as pl
from jax.experimental.pallas import tpu as pltpu
from jax.sharding import PartitionSpec as P

LN_EPS = 1e-05
RMS_EPS = 1e-06


def shifted(value, axis, by):
    size = lax.axis_size(axis)
    pairs = [(i, i + by) for i in range(size) if 0 <= i + by < size]
    return lax.ppermute(value, axis, pairs)


def body_slots(
    resid,
    a_val,
    a_gate,
    conv_kernel,
    conv_bias,
    ln_gain,
    ln_bias,
    w_out,
    ffn_gain,
    routes,
    route_weights,
    exp_gate,
    exp_up,
    exp_down,
    sh_gate,
    sh_up,
    sh_down,
):
    tp_count = lax.axis_size("tp")
    tp_place = lax.axis_index("tp")
    sp_count = lax.axis_size("sp")
    tok_rows = resid.shape[0]
    model_width = resid.shape[1]
    col_width = model_width // tp_count
    col_start = tp_place * col_width
    conv_span = conv_kernel.shape[0]
    channels_all = a_val.shape[1] * tp_count
    gated_in = (a_val.astype(jnp.float32) * jax.nn.sigmoid(a_gate.astype(jnp.float32))).astype(
        jnp.bfloat16
    )
    before = shifted(gated_in[tok_rows - (conv_span - 1) :], "sp", 1)
    padded = jnp.concatenate([before, gated_in], axis=0).astype(jnp.float32)
    kernel = conv_kernel.astype(jnp.float32)

    def add_tap(offset, running):
        window_rows = lax.dynamic_slice_in_dim(padded, offset, tok_rows, 0)
        return running + lax.dynamic_slice_in_dim(kernel, offset, 1, 0) * window_rows

    start_sum = jnp.broadcast_to(conv_bias[None, :], gated_in.shape)
    conv_out = lax.fori_loop(0, conv_span, add_tap, start_sum)
    row_sums = lax.psum((jnp.sum(conv_out, axis=1), jnp.sum(conv_out * conv_out, axis=1)), "tp")
    channel_mean = row_sums[0] / channels_all
    channel_var = row_sums[1] / channels_all - channel_mean * channel_mean
    scaled = (conv_out - channel_mean[:, None]) * lax.rsqrt(
        channel_var[:, None] + LN_EPS
    ) * ln_gain[None, :] + ln_bias[None, :]
    mixed_out = jax.nn.silu(scaled).astype(jnp.bfloat16)
    partial_proj = jnp.dot(mixed_out, w_out, preferred_element_type=jnp.float32)
    projected = lax.psum(partial_proj, "tp")
    middle = (resid.astype(jnp.float32) + projected).astype(jnp.bfloat16)
    middle_f = middle.astype(jnp.float32)
    inverse = lax.rsqrt(jnp.mean(middle_f * middle_f, axis=1, keepdims=True) + RMS_EPS)
    normed = (middle_f * inverse * ffn_gain[None, :]).astype(jnp.bfloat16)
    middle_cols = lax.dynamic_slice_in_dim(middle, col_start, col_width, 1)
    shared_gate = jnp.dot(normed, sh_gate, preferred_element_type=jnp.float32)
    shared_up = jnp.dot(normed, sh_up, preferred_element_type=jnp.float32)
    shared_hidden = (jax.nn.silu(shared_gate) * shared_up).astype(jnp.bfloat16)
    weight_rows = sh_down
    shared = jnp.dot(
        lax.all_gather(shared_hidden, "tp", axis=1, tiled=True),
        weight_rows,
        preferred_element_type=jnp.float32,
    )
    top_count = routes.shape[1]
    local_experts = exp_gate.shape[0]
    experts_all = local_experts * sp_count
    capacity = max(2 * tok_rows * top_count // experts_all, tp_count)
    pair_count = tok_rows * top_count
    chosen = routes.reshape(pair_count)
    one_hot = (chosen[:, None] == jnp.arange(experts_all, dtype=jnp.int32)[None, :]).astype(
        jnp.int32
    )
    earlier = jnp.cumsum(one_hot, axis=0) - one_hot
    place_in = jnp.sum(earlier * one_hot, axis=1)
    slot_of = chosen * capacity + place_in
    owner_ids = (
        jnp.zeros((experts_all * capacity,), jnp.int32)
        .at[slot_of]
        .set(jnp.arange(pair_count, dtype=jnp.int32) + 1)
    )
    owner_grid = owner_ids.reshape(sp_count, local_experts, capacity)
    part_slots = capacity // tp_count
    own_owners = lax.dynamic_slice_in_dim(owner_grid, tp_place * part_slots, part_slots, 2)
    source_row = jnp.maximum(own_owners - 1, 0) // top_count
    taken = normed[source_row.reshape(-1)].reshape(own_owners.shape + (model_width,))
    landed = lax.all_to_all(
        jnp.where((own_owners > 0)[..., None], taken, jnp.zeros((), jnp.bfloat16)),
        "sp",
        split_axis=0,
        concat_axis=0,
        tiled=True,
    )
    arrived = lax.all_gather(landed, "tp", axis=2, tiled=True)
    gate_part = jnp.einsum("sxcd,xdf->sxcf", arrived, exp_gate, preferred_element_type=jnp.float32)
    up_part = jnp.einsum("sxcd,xdf->sxcf", arrived, exp_up, preferred_element_type=jnp.float32)
    expert_hidden = (jax.nn.silu(gate_part) * up_part).astype(jnp.bfloat16)
    weight_rows = exp_down
    expert_sum = jnp.einsum(
        "sxcf,xfd->sxcd",
        lax.all_gather(expert_hidden, "tp", axis=3, tiled=True),
        weight_rows,
        preferred_element_type=jnp.float32,
    )
    expert_out = expert_sum.astype(jnp.bfloat16)
    returned = lax.all_to_all(expert_out, "sp", split_axis=0, concat_axis=0, tiled=True)
    flat_out = returned.reshape(experts_all * capacity, col_width)
    picked = flat_out[slot_of].astype(jnp.float32).reshape(tok_rows, top_count, col_width)
    routed = jnp.sum(picked * route_weights[:, :, None], axis=1)
    return (middle_cols.astype(jnp.float32) + shared + routed).astype(jnp.bfloat16)


def swapped(value, axis, bit):
    size = lax.axis_size(axis)
    return lax.ppermute(value, axis, [(i, i ^ bit) for i in range(size)])


def gather_kernel(
    levels,
    own_ref,
    weight_ref,
    down_ref,
    rows_ref,
    weights_ref,
    swap_ref,
    local_sem,
    up_sem,
    low_sem,
    side_sem,
    core_sem,
    main_recv,
    core_recv,
    weight_send,
    weight_recv,
    swap_sem,
):
    count = 2 * levels
    me = lax.axis_index("sp")
    tp_place = lax.axis_index("tp")
    level, side = me // 2, me % 2
    row, core = tp_place // 2, tp_place % 2
    core_peer = {"tp": row * 2 + (1 - core)}
    row_peer = {"tp": (1 - row) * 2 + core}
    side_peer = {"sp": level * 2 + (1 - side)}
    mesh_ids = pl.DeviceIdType.MESH

    barrier = pltpu.get_barrier_semaphore()
    others = [lax.rem(me + step, count) for step in range(1, count)]
    for other in others:
        pl.semaphore_signal(barrier, inc=1, device_id={"sp": other}, device_id_type=mesh_ids)
    pl.semaphore_signal(barrier, inc=1, device_id=core_peer, device_id_type=mesh_ids)
    pl.semaphore_signal(barrier, inc=1, device_id=row_peer, device_id_type=mesh_ids)
    pl.semaphore_wait(barrier, count + 1)

    def remote(src, dst, send, recv, where):
        return pltpu.make_async_remote_copy(
            src_ref=src, dst_ref=dst, send_sem=send, recv_sem=recv, device_id=where, device_id_type=mesh_ids
        )

    def block(at):
        return rows_ref.at[core, at]

    half_rows = swap_ref.shape[0]
    swap = remote(
        down_ref.at[0, pl.ds(pl.multiple_of((1 - row) * half_rows, half_rows), half_rows)],
        swap_ref,
        swap_sem.at[0],
        swap_sem.at[1],
        row_peer,
    )

    def up_copy(src, origin):
        at = origin * 2 + side
        return remote(src, block(at), up_sem.at[origin], main_recv.at[at], {"sp": me + 2})

    def low_copy(src, origin):
        at = origin * 2 + side
        return remote(src, block(at), low_sem.at[origin], main_recv.at[at], {"sp": me - 2})

    def side_copy(src, origin):
        at = origin * 2 + side
        return remote(src, block(at), side_sem.at[origin], main_recv.at[at], side_peer)

    def core_copy(src, at):
        return remote(src, block(at), core_sem.at[at], core_recv.at[at], core_peer)

    def landed(at):
        remote(block(at), block(at), core_sem.at[at], main_recv.at[at], core_peer).wait_recv()

    @pl.when(level < levels - 1)
    def _():
        up_copy(own_ref, level).start()

    @pl.when(level > 0)
    def _():
        low_copy(own_ref, level).start()

    side_copy(own_ref, level).start()
    swap.start()
    core_copy(own_ref, me).start()
    weight_copies = [
        remote(
            weight_ref,
            weights_ref.at[me],
            weight_send.at[step],
            weight_recv.at[me],
            {"sp": other},
        )
        for step, other in enumerate(others)
    ]
    for copy in weight_copies:
        copy.start()
    keep = pltpu.make_async_copy(own_ref, block(me), local_sem.at[0])
    keep.start()
    keep_weight = pltpu.make_async_copy(weight_ref, weights_ref.at[me], local_sem.at[1])
    keep_weight.start()

    for step in range(1, levels):
        below = level - step
        above = level + step

        @pl.when(below >= 0)
        def _():
            at = below * 2 + side
            landed(at)

            @pl.when(level < levels - 1)
            def _():
                up_copy(block(at), below).start()

            side_copy(block(at), below).start()
            core_copy(block(at), at).start()

        @pl.when(above < levels)
        def _():
            at = above * 2 + side
            landed(at)

            @pl.when(level > 0)
            def _():
                low_copy(block(at), above).start()

            side_copy(block(at), above).start()
            core_copy(block(at), at).start()

    def from_side(origin):
        at = origin * 2 + (1 - side)
        landed(at)
        core_copy(block(at), at).start()

    from_side(level)
    for step in range(1, levels):
        below = level - step
        above = level + step

        @pl.when(below >= 0)
        def _():
            from_side(below)

        @pl.when(above < levels)
        def _():
            from_side(above)

    keep.wait()
    keep_weight.wait()
    for copy in weight_copies:
        copy.wait_send()
    for other in others:
        remote(
            weight_ref, weights_ref.at[other], weight_send.at[0], weight_recv.at[other], core_peer
        ).wait_recv()
    for origin in range(levels):
        side_copy(own_ref, origin).wait_send()

        @pl.when((level < levels - 1) & (origin <= level))
        def _():
            up_copy(own_ref, origin).wait_send()

        @pl.when((level > 0) & (origin >= level))
        def _():
            low_copy(own_ref, origin).wait_send()

    for at in range(count):
        core_copy(own_ref, at).wait_send()
        far = rows_ref.at[1 - core, at]
        remote(far, far, core_sem.at[at], core_recv.at[at], core_peer).wait_recv()
    swap.wait()


def gather_rows(mid_half, weight_rows, down, half_rows):
    count = lax.axis_size("sp")
    levels = count // 2
    tok_rows, half_width = mid_half.shape
    vmem = pl.BlockSpec(memory_space=pltpu.VMEM)
    hbm = pl.BlockSpec(memory_space=pltpu.HBM)
    dma = pltpu.SemaphoreType.DMA
    return pl.pallas_call(
        functools.partial(gather_kernel, levels),
        out_shape=(
            jax.ShapeDtypeStruct((2, count, tok_rows, half_width), mid_half.dtype),
            jax.ShapeDtypeStruct((count,) + weight_rows.shape, weight_rows.dtype),
            jax.ShapeDtypeStruct((half_rows, down.shape[2]), down.dtype),
        ),
        in_specs=[vmem, vmem, hbm],
        out_specs=(vmem, vmem, hbm),
        scratch_shapes=[
            dma((2,)),
            dma((levels,)),
            dma((levels,)),
            dma((levels,)),
            dma((count,)),
            dma((count,)),
            dma((count,)),
            dma((count - 1,)),
            dma((count,)),
            dma((2,)),
        ],
        compiler_params=pltpu.CompilerParams(
            collective_id=0, has_side_effects=True, vmem_limit_bytes=24 * 1024 * 1024
        ),
    )(mid_half, weight_rows, down)


def body_dense(
    resid,
    a_val,
    a_gate,
    conv_kernel,
    conv_bias,
    ln_gain,
    ln_bias,
    w_out,
    ffn_gain,
    routes,
    route_weights,
    exp_gate,
    exp_up,
    exp_down,
    sh_gate,
    sh_up,
    sh_down,
):
    tp_count = lax.axis_size("tp")
    tp_place = lax.axis_index("tp")
    core = tp_place % 2
    row = tp_place // 2
    sp_count = lax.axis_size("sp")
    tok_rows, model_width = resid.shape
    col_width = model_width // tp_count
    half_width = model_width // 2
    part_hidden = exp_gate.shape[2]
    conv_span = conv_kernel.shape[0]
    channels_all = a_val.shape[1] * tp_count

    gated_in = (a_val.astype(jnp.float32) * jax.nn.sigmoid(a_gate.astype(jnp.float32))).astype(
        jnp.bfloat16
    )
    before = shifted(gated_in[tok_rows - (conv_span - 1) :], "sp", 1)
    expert_ids = jnp.arange(sp_count, dtype=jnp.int32)
    weight_mat = jnp.sum(
        jnp.where(routes[:, :, None] == expert_ids[None, None, :], route_weights[:, :, None], 0.0),
        axis=1,
    )
    padded = jnp.concatenate([before, gated_in], axis=0).astype(jnp.float32)
    kernel = conv_kernel.astype(jnp.float32)
    conv_out = jnp.broadcast_to(conv_bias[None, :], gated_in.shape)
    for tap in range(conv_span):
        conv_out = conv_out + kernel[tap : tap + 1] * padded[tap : tap + tok_rows]
    row_sums = lax.psum((jnp.sum(conv_out, axis=1), jnp.sum(conv_out * conv_out, axis=1)), "tp")
    channel_mean = row_sums[0] / channels_all
    channel_var = row_sums[1] / channels_all - channel_mean * channel_mean
    scaled = (conv_out - channel_mean[:, None]) * lax.rsqrt(
        channel_var[:, None] + LN_EPS
    ) * ln_gain[None, :] + ln_bias[None, :]
    mixed_out = jax.nn.silu(scaled).astype(jnp.bfloat16)
    partial_proj = jnp.dot(mixed_out, w_out, preferred_element_type=jnp.float32)
    give = lax.dynamic_slice_in_dim(partial_proj, (1 - core) * half_width, half_width, 1)
    keep = lax.dynamic_slice_in_dim(partial_proj, core * half_width, half_width, 1)
    chip_sum = keep + swapped(give.astype(jnp.bfloat16), "tp", 1).astype(jnp.float32)
    chip_sum = chip_sum.astype(jnp.bfloat16)
    half_sum = chip_sum.astype(jnp.float32) + swapped(chip_sum, "tp", 2).astype(jnp.float32)
    resid_half = lax.dynamic_slice_in_dim(resid, core * half_width, half_width, 1)
    mid_half = (resid_half.astype(jnp.float32) + half_sum).astype(jnp.bfloat16)
    gathered, weights_got, swapped_down = gather_rows(
        mid_half, weight_mat.T, exp_down, 2 * part_hidden
    )
    sp_place = lax.axis_index("sp")
    weight_own = lax.dynamic_index_in_dim(weights_got, sp_place, 1, False).reshape(-1, 1)
    own_halves = lax.dynamic_index_in_dim(gathered, sp_place, 1, False)
    middle = jnp.concatenate([own_halves[0], own_halves[1]], axis=1)

    middle_f = middle.astype(jnp.float32)
    inverse = lax.rsqrt(jnp.mean(middle_f * middle_f, axis=1, keepdims=True) + RMS_EPS)
    normed = (middle_f * inverse * ffn_gain[None, :]).astype(jnp.bfloat16)
    middle_cols = lax.dynamic_slice_in_dim(middle, tp_place * col_width, col_width, 1)
    shared_gate = jnp.dot(normed, sh_gate, preferred_element_type=jnp.float32)
    shared_up = jnp.dot(normed, sh_up, preferred_element_type=jnp.float32)
    shared_hidden = (jax.nn.silu(shared_gate) * shared_up).astype(jnp.bfloat16)
    shared = jnp.dot(
        lax.all_gather(shared_hidden, "tp", axis=1, tiled=True),
        sh_down,
        preferred_element_type=jnp.float32,
    )

    all_rows = sp_count * tok_rows
    rows_f = jnp.concatenate(
        [gathered[0].reshape(all_rows, half_width), gathered[1].reshape(all_rows, half_width)], axis=1
    ).astype(jnp.float32)
    rows_inverse = lax.rsqrt(jnp.mean(rows_f * rows_f, axis=1, keepdims=True) + RMS_EPS)
    rows = (rows_f * rows_inverse * ffn_gain[None, :]).astype(jnp.bfloat16)
    gate_part = jnp.dot(rows, exp_gate[0], preferred_element_type=jnp.float32)
    up_part = jnp.dot(rows, exp_up[0], preferred_element_type=jnp.float32)
    hidden = (jax.nn.silu(gate_part) * up_part).astype(jnp.bfloat16)
    hidden_peer = swapped(hidden, "tp", 1)

    own_at = tp_place * part_hidden
    peer_at = (tp_place ^ 1) * part_hidden
    stay = lax.dynamic_slice_in_dim
    out_far = jnp.dot(
        hidden, stay(swapped_down, core * part_hidden, part_hidden, 0), preferred_element_type=jnp.float32
    ) + jnp.dot(
        hidden_peer,
        stay(swapped_down, (1 - core) * part_hidden, part_hidden, 0),
        preferred_element_type=jnp.float32,
    )
    far = swapped((out_far * weight_own).astype(jnp.bfloat16), "tp", 2)
    out_own = jnp.dot(
        hidden, stay(exp_down[0], own_at, part_hidden, 0), preferred_element_type=jnp.float32
    ) + jnp.dot(
        hidden_peer, stay(exp_down[0], peer_at, part_hidden, 0), preferred_element_type=jnp.float32
    )
    expert_sum = (out_own * weight_own + far.astype(jnp.float32)).astype(jnp.bfloat16)
    returned = lax.all_to_all(
        expert_sum.reshape(sp_count, tok_rows, col_width), "sp", split_axis=0, concat_axis=0, tiled=True
    )
    routed = jnp.sum(returned.astype(jnp.float32), axis=0)
    return (middle_cols.astype(jnp.float32) + shared + routed).astype(jnp.bfloat16)


def body(*args):
    tok_rows = args[0].shape[0]
    top_count = args[9].shape[1]
    local_experts = args[11].shape[0]
    experts_all = local_experts * lax.axis_size("sp")
    capacity = 2 * tok_rows * top_count // experts_all
    if (
        local_experts == 1
        and lax.axis_size("tp") == 4
        and lax.axis_size("sp") % 2 == 0
        and capacity >= tok_rows
    ):
        return body_dense(*args)
    return body_slots(*args)


def solution(mesh):
    in_specs = (
        P("sp", None),
        P("sp", "tp"),
        P("sp", "tp"),
        P(None, "tp"),
        P("tp"),
        P("tp"),
        P("tp"),
        P("tp", None),
        P(),
        P("sp", None),
        P("sp", None),
        P("sp", None, "tp"),
        P("sp", None, "tp"),
        P("sp", None, "tp"),
        P(None, "tp"),
        P(None, "tp"),
        P(None, "tp"),
    )
    out_specs = P("sp", "tp")
    return jax.shard_map(body, mesh=mesh, in_specs=in_specs, out_specs=out_specs, check_vma=False)
```
